32 devices in a mesh: sp: 16 (over z, y, x), tp: 2 (over core).
Axes of the slice: x: 2, y: 2, z: 4, core: 2. Of those that a mesh axis runs over, the one named last changes fastest.
Arguments:
- tokens: bfloat16 [4096, 4096], P('sp'), may hold values from -5 to 5
- documents: int32 [4096], P('sp'), may hold values from 0 to 3, never falling along the last dimension, each value on 1 to 2048 neighbouring positions
- norm_gain: float32 [2, 4096], replicated, may hold values from 0.1 to 1.9
- in_weight: bfloat16 [2, 4096, 2048], P(None, 'sp', 'tp'), may hold values from -0.09375 to 0.09375
- conv_taps: float32 [2, 4, 2048], P(None, None, 'tp'), may hold values from -3 to 3
- conv_bias: float32 [2, 2048], P(None, 'tp'), may hold values from -0.75 to 0.75
- recur_gate: bfloat16 [2, 32, 64, 64], P(None, 'tp'), may hold values from -0.75 to 0.75
- input_gate: bfloat16 [2, 32, 64, 64], P(None, 'tp'), may hold values from -0.75 to 0.75
- recur_bias: float32 [2, 2048], P(None, 'tp'), may hold values from -4 to 4
- input_bias: float32 [2, 2048], P(None, 'tp'), may hold values from -4 to 4
- decay_param: float32 [2, 2048], P(None, 'tp'), may hold values from 4 to 7
- out_weight: bfloat16 [2, 2048, 4096], P(None, 'tp', 'sp'), may hold values from -0.375 to 0.375
Outputs:
- layered: bfloat16 [4096, 4096], P('sp')
The draws below stay inside these ranges and needn't reach their ends.
All inputs are finite; a program needn't handle non-finite values.
Results may differ from the reference program's by a relative error of at most 0.017.
Values may be sent and summed in bfloat16 or wider, within the bound.
No kernel may reach another device: no remote copies, remote signals or barrier semaphores. Data moves between devices by JAX's collectives and lax.ppermute only.
A program may use at most 128 MiB of HBM per device.

```python
import math
import jax
import jax.numpy as jnp
import numpy as np
from jax import lax

D = 4096
RW = 2048
BD = 64
K = 4
LAYERS = 2
TOK_DEV = 256
TOKENS = 4096
NB = 32
N_SP = 16
N_TP = 2


def draw_tokens(key, part):
    scale_key, value_key, mean_key = jax.random.split(jax.random.fold_in(key, 11), 3)
    log_scale = jax.random.uniform(scale_key, (TOKENS // 128, 1), jnp.float32, -1.3863, -0.2877)
    block_scale = jnp.repeat(jnp.exp(log_scale), 128, axis=0)
    base = jax.random.normal(value_key, (TOKENS, D), jnp.float32)
    base = jnp.clip(base, -6.0, 6.0)
    return (base * block_scale).astype(jnp.bfloat16)


def draw_decay_param(key, part):
    flag_key, slow_key, fast_key = jax.random.split(jax.random.fold_in(key, 23), 3)
    picked = jax.random.randint(flag_key, (LAYERS, RW), 0, 2)
    slow_value = jax.random.uniform(slow_key, (LAYERS, RW), jnp.float32, 6.5, 7.0)
    fast_value = jax.random.uniform(fast_key, (LAYERS, RW), jnp.float32, 4.0, 5.0)
    return jnp.where(picked == 0, fast_value, slow_value)


def shard_levels(own_key, extent, pieces, smallest, high):
    gain = 1.0
    for dim, parts in pieces:
        draws = jax.random.uniform(jax.random.fold_in(jax.random.fold_in(own_key, 6), dim), (parts,), jnp.float32, smallest / len(pieces), high / len(pieces))
        gain = gain * jnp.repeat(jnp.exp(draws), extent[dim] // parts).reshape((-1,) + (1,) * (len(extent) - 1 - dim))
    return gain


def split_up(number_of, total, bound, lean):
    portions = [(1 << 20) // math.isqrt(standing ** lean) + 1 for standing in range(2, number_of + 1)]
    surplus, holding = total - bound - (number_of - 1), [1] * (number_of - 1)
    while surplus > 0:
        movable = [i for i in range(number_of - 1) if holding[i] < bound]
        mass, budget = sum([portions[i] for i in movable]), surplus
        for i in movable:
            addition = min(bound - holding[i], max(1, budget * portions[i] // mass), surplus)
            holding[i] = holding[i] + addition
            surplus = surplus - addition
    return np.array([bound] + holding)


def ragged(rng, number_of, total, most, slope):
    if number_of == 2:
        one = jax.random.randint(rng, (), max(1, total - most), min(most, total - 1) + 1)
        return jnp.stack([one, total - one])
    lengths = jnp.asarray(split_up(number_of, total, most, slope), jnp.int32)
    twos = (number_of - 1) // 2
    donor, sink = lengths[1:1 + 2 * twos:2], lengths[2:2 + 2 * twos:2]
    margin = jnp.minimum(donor - 1, most - sink)
    moved = jax.random.randint(jax.random.fold_in(rng, 1), (twos,), 0, 1 << 20) % (margin + 1)
    lengths = lengths.at[1:1 + 2 * twos:2].set(donor - moved).at[2:2 + 2 * twos:2].set(sink + moved)
    return lengths[jax.random.permutation(jax.random.fold_in(rng, 2), number_of)]


def bell_draw(rng, shape, scale, most, shards=(), kind=jnp.bfloat16):
    drawn = jax.random.normal(rng, shape, jnp.float32) * scale
    if len(shards) > 0:
        drawn = shard_levels(rng, shape, shards, -0.22, 0.18) * drawn
    return jnp.clip(drawn, min=-most, max=most).astype(kind)


def setup_inputs(seed: int = 0) -> dict:
    splits = jax.random.split(jax.random.key(seed), 13)
    tokens = draw_tokens(jax.random.fold_in(splits[12], 71), 0)
    documents = jnp.searchsorted(jnp.cumsum(ragged(splits[1], N_SP // 4, TOKENS, 8 * TOK_DEV, 0)), jnp.arange(TOKENS), side="right").astype(jnp.int32)
    norm_gain = jnp.clip(1.0 + 0.18 * jax.random.normal(splits[2], (LAYERS, D), jnp.float32), 0.1, 1.9)
    in_weight = bell_draw(splits[3], (LAYERS, D, RW), D ** -0.5, 0.09375, ((1, 16), (2, 2)))
    conv_taps = bell_draw(splits[4], (LAYERS, K, RW), K ** -0.5, 3.0, ((2, 2),), jnp.float32)
    conv_bias = bell_draw(splits[5], (LAYERS, RW), 0.05, 0.75, ((1, 2),), jnp.float32)
    recur_gate = bell_draw(splits[6], (LAYERS, NB, BD, BD), BD ** -0.5, 0.75, ((1, 2),))
    input_gate = bell_draw(splits[7], (LAYERS, NB, BD, BD), BD ** -0.5, 0.75, ((1, 2),))
    recur_bias = bell_draw(splits[8], (LAYERS, RW), 1.0, 4.0, ((1, 2),), jnp.float32)
    input_bias = bell_draw(splits[9], (LAYERS, RW), 1.0, 4.0, ((1, 2),), jnp.float32)
    decay_param = draw_decay_param(jax.random.fold_in(splits[12], 71), 0)
    out_weight = bell_draw(splits[11], (LAYERS, RW, D), (RW // 8) ** -0.5, 0.375, ((1, 2), (2, 16)))
    return {"tokens": tokens, "documents": documents, "norm_gain": norm_gain, "in_weight": in_weight, "conv_taps": conv_taps, "conv_bias": conv_bias, "recur_gate": recur_gate, "input_gate": input_gate, "recur_bias": recur_bias, "input_bias": input_bias, "decay_param": decay_param, "out_weight": out_weight}


RG_C = 8.0
EPS = 0.1

def norm_rows(values_in, gain_row):
    values = values_in.astype(jnp.float32)
    scaled = values * lax.rsqrt(lax.optimization_barrier(jnp.mean(values * values, axis=-1, keepdims=True)) + EPS)
    return (scaled * gain_row[None, :]).astype(jnp.bfloat16)

def combine(earlier, following):
    return (earlier[0] * following[0], following[0] * earlier[1] + following[1])

def reference(tokens, documents, norm_gain, in_weight, conv_taps, conv_bias, recur_gate, input_gate, recur_bias, input_bias, decay_param, out_weight):
    state_x = tokens
    prev_doc = jnp.concatenate([documents[:1], documents[:-1]])
    reset = documents != prev_doc
    group_width = RW // N_TP
    for depth_at in range(LAYERS):
        normed = norm_rows(state_x, norm_gain[depth_at])
        mixed_in = jnp.dot(normed, in_weight[depth_at], preferred_element_type=jnp.float32).astype(jnp.bfloat16)
        values_in = mixed_in.astype(jnp.float32)
        conv_sum = conv_bias[depth_at][None, :] + conv_taps[depth_at, 0][None, :] * values_in
        for lag_step in range(1, K):
            shifted = jnp.concatenate([jnp.zeros((lag_step, RW), jnp.float32), values_in[:-lag_step]], axis=0)
            shifted_doc = jnp.concatenate([jnp.full((lag_step,), -1, jnp.int32), documents[:-lag_step]], axis=0)
            same_doc = (shifted_doc == documents)[:, None]
            conv_sum = conv_sum + jnp.where(same_doc, conv_taps[depth_at, lag_step][None, :] * shifted, 0.0)
        conv_out = conv_sum.astype(jnp.bfloat16)
        grouped = conv_out.astype(jnp.float32).reshape(TOKENS, NB, BD)
        recur_rate = jax.nn.sigmoid(jnp.einsum('snb,nbc->snc', grouped, recur_gate[depth_at].astype(jnp.float32)).reshape(TOKENS, RW) + recur_bias[depth_at][None, :])
        input_rate = jax.nn.sigmoid(jnp.einsum('snb,nbc->snc', grouped, input_gate[depth_at].astype(jnp.float32)).reshape(TOKENS, RW) + input_bias[depth_at][None, :])
        log_decay = -RG_C * jax.nn.softplus(-decay_param[depth_at])[None, :] * recur_rate
        decay_now = jnp.where(reset[:, None], 0.0, jnp.exp(log_decay))
        drive_term = jnp.sqrt(jnp.maximum(-jnp.expm1(2.0 * log_decay), 0.0)) * (input_rate * conv_out.astype(jnp.float32))
        _, states = lax.associative_scan(combine, (decay_now, drive_term), axis=0)
        hidden = states.astype(jnp.bfloat16)
        summed = jnp.zeros((TOKENS, D), jnp.float32)
        for group in range(N_TP):
            low = group * group_width
            partial_term = jnp.dot(hidden[:, low:low + group_width], out_weight[depth_at, low:low + group_width], preferred_element_type=jnp.float32).astype(jnp.bfloat16)
            partial_term = lax.optimization_barrier(partial_term)
            summed = summed + partial_term.astype(jnp.float32)
        state_x = (state_x.astype(jnp.float32) + summed).astype(jnp.bfloat16)
    return state_x
```

```python
import functools
import jax
import jax.numpy as jnp
from jax import lax
from jax.experimental import pallas as pl
from jax.experimental.pallas import tpu as pltpu
from jax.sharding import Mesh, PartitionSpec as P

RG_C = 8.0
EPS = 0.1
SUB = 8
F32 = jnp.float32
BF16 = jnp.bfloat16
VMEM_LIMIT = 48 * 1024 * 1024


def vmem():
    return pl.BlockSpec(memory_space=pltpu.VMEM)


def params(**kw):
    return pltpu.CompilerParams(vmem_limit_bytes=VMEM_LIMIT, **kw)


def in_kernel(groups, adds, x_ref, *refs):
    y_refs, (gain_ref, w_ref), outs = refs[:adds], refs[adds : adds + 2], refs[adds + 2 :]
    if adds:
        new_ref, outs = outs[0], outs[1:]
    ss_ref, m_refs = outs[0], outs[1:]
    slices, rows, width = x_ref.shape
    lanes = min(width, 128)
    squares = jnp.zeros((rows, lanes), F32)
    scaled = []
    for z in range(slices):
        value = x_ref[z].astype(F32)
        if adds:
            summed = y_refs[0][z].astype(F32)
            for y_ref in y_refs[1:]:
                summed = summed + y_ref[z].astype(F32)
            rounded = (value + summed).astype(BF16)
            new_ref[z] = rounded
            value = rounded.astype(F32)
        square = value * value
        for low in range(0, width, lanes):
            squares = squares + square[:, low : low + lanes]
        scaled.append((value * gain_ref[z]).astype(BF16))
    for low in range(0, rows, 128):
        ss_ref[0, :, low : low + 128] = jnp.sum(squares[low : low + 128].T, axis=0, keepdims=True)
    for k in range(groups):
        total = jnp.dot(scaled[0], w_ref[0, k], preferred_element_type=F32)
        for z in range(1, slices):
            total = total + jnp.dot(scaled[z], w_ref[z, k], preferred_element_type=F32)
        m_refs[k][...] = total.astype(BF16)


def in_projection(x, ys, gain, w):
    slices, rows, width = x.shape
    groups, chans = w.shape[1], w.shape[3]
    tile = min(rows, 256)
    count = rows // tile
    row_block = pl.BlockSpec((slices, tile, width), lambda i: (0, i, 0))
    out_shape = [jax.ShapeDtypeStruct((count, 1, tile), F32)]
    out_specs = [pl.BlockSpec((1, 1, tile), lambda i: (i, 0, 0))]
    for _ in range(groups):
        out_shape.append(jax.ShapeDtypeStruct((rows, chans), BF16))
        out_specs.append(pl.BlockSpec((tile, chans), lambda i: (i, 0)))
    if ys:
        out_shape.insert(0, jax.ShapeDtypeStruct(x.shape, BF16))
        out_specs.insert(0, row_block)
    got = pl.pallas_call(
        functools.partial(in_kernel, groups, len(ys)),
        grid=(count,),
        in_specs=[row_block] * (1 + len(ys))
        + [
            pl.BlockSpec(gain.shape, lambda i: (0, 0, 0)),
            pl.BlockSpec(w.shape, lambda i: (0, 0, 0, 0)),
        ],
        out_specs=out_specs,
        out_shape=out_shape,
        compiler_params=params(),
        name="in_projection",
    )(x, *ys, gain, w)
    if ys:
        return got[0], got[1], got[2:]
    return x, got[0], got[1:]


def mix_kernel(groups, features, *refs):
    m_refs, s_refs, (mixed_ref, tail_ref) = refs[:groups], refs[groups : 2 * groups], refs[2 * groups :]
    rows, chans = mixed_ref.shape
    count, _, tile = s_refs[0].shape
    lanes = min(chans, 128)
    for n in range(count):
        stat = s_refs[0][n]
        for s_ref in s_refs[1:]:
            stat = stat + s_ref[n]
        factor = lax.rsqrt(stat * (1.0 / features) + EPS)
        for low in range(0, tile, 128):
            column = jnp.broadcast_to(factor[:, low : low + 128], (128, 128)).T
            at = n * tile + low
            for lane in range(0, chans, lanes):
                total = m_refs[0][at : at + 128, lane : lane + lanes].astype(F32)
                for m_ref in m_refs[1:]:
                    total = total + m_ref[at : at + 128, lane : lane + lanes].astype(F32)
                mixed_ref[at : at + 128, lane : lane + lanes] = (total * column[:, :lanes]).astype(BF16)
    last = mixed_ref[rows - 4 * SUB :, :].astype(F32)
    ends = [last[j * SUB + SUB - 1 : (j + 1) * SUB, :] for j in range(4)]
    tail_ref[...] = jnp.concatenate(ends + ends, axis=0)


def mix(pieces, stats, features):
    rows, chans = pieces[0].shape
    return pl.pallas_call(
        functools.partial(mix_kernel, len(pieces), features),
        in_specs=[vmem()] * (2 * len(pieces)),
        out_specs=[vmem(), vmem()],
        out_shape=[
            jax.ShapeDtypeStruct((rows, chans), BF16),
            jax.ShapeDtypeStruct((SUB, chans), F32),
        ],
        compiler_params=params(),
        name="mix",
    )(*pieces, *stats)


def recur_kernel(
    taps_count, mixed_ref, halo_ref, keep_ref, table_ref, gate_ref,
    cum_ref, state_ref, head_ref, ext_ref, conv_ref, pre_ref,
):
    rows, chans = mixed_ref.shape
    lead = (taps_count - 1) * SUB
    tile = 64
    ext_ref[lead:, :] = mixed_ref[...].astype(F32)
    for j in range(taps_count - 1):
        back = taps_count - 1 - j
        end = ext_ref[lead + rows - back * SUB : lead + rows - (back - 1) * SUB, :]
        ext_ref[j * SUB : (j + 1) * SUB, :] = jnp.concatenate(
            [halo_ref[4 - back : 5 - back, :], end[: SUB - 1]], axis=0
        )

    def conv(step, _):
        at = pl.multiple_of(step * tile, tile)
        total = table_ref[taps_count : taps_count + 1, :] + table_ref[0:1, :] * ext_ref[
            pl.ds(at + lead, tile), :
        ]
        for lag in range(1, taps_count):
            total = total + keep_ref[pl.ds(at, tile), lag - 1 : lag] * (
                table_ref[lag : lag + 1, :] * ext_ref[pl.ds(at + lead - lag * SUB, tile), :]
            )
        conv_ref[pl.ds(at, tile), :] = total.astype(BF16)
        return 0

    lax.fori_loop(0, rows // tile, conv, 0)
    pre_ref[...] = jnp.dot(conv_ref[...], gate_ref[...], preferred_element_type=F32)
    base = taps_count + 1

    def scan(step, carry):
        cum, state = carry
        at = pl.multiple_of(step * tile, tile)
        recur_rate = jax.nn.sigmoid(pre_ref[pl.ds(at, tile), :chans] + table_ref[base : base + 1, :])
        input_rate = jax.nn.sigmoid(
            pre_ref[pl.ds(at, tile), chans:] + table_ref[base + 1 : base + 2, :]
        )
        log_decay = table_ref[base + 2 : base + 3, :] * recur_rate
        decay = jnp.exp(log_decay)
        twice = 2.0 * log_decay
        near = -twice * (1.0 + twice * (0.5 + twice * (1.0 / 6.0 + twice * (1.0 / 24.0))))
        rest = jnp.where(twice > -0.03, near, 1.0 - decay * decay)
        drive = jnp.sqrt(jnp.maximum(rest, 0.0)) * (
            input_rate * conv_ref[pl.ds(at, tile), :].astype(F32)
        )
        decay = keep_ref[pl.ds(at, tile), 0:1] * decay
        cums, states = [], []
        for i in range(tile // SUB):
            now = decay[i * SUB : (i + 1) * SUB]
            cum = cum * now
            state = state * now + drive[i * SUB : (i + 1) * SUB]
            cums.append(cum)
            states.append(state)
        cum_ref[pl.ds(at, tile), :] = jnp.concatenate(cums, axis=0)
        state_ref[pl.ds(at, tile), :] = jnp.concatenate(states, axis=0)
        return cum, state

    cum, state = lax.fori_loop(
        0, rows // tile, scan, (jnp.ones((SUB, chans), F32), jnp.zeros((SUB, chans), F32))
    )
    decays, states = [jnp.ones((1, chans), F32)], [jnp.zeros((1, chans), F32)]
    for s in range(SUB):
        decays.append(decays[-1] * cum[s : s + 1])
        states.append(states[-1] * cum[s : s + 1] + state[s : s + 1])
    head_ref[0:SUB, :] = jnp.concatenate(decays[:SUB], axis=0)
    head_ref[SUB : 2 * SUB, :] = jnp.concatenate(states[:SUB], axis=0)
    head_ref[2 * SUB :, :] = jnp.concatenate([decays[SUB], states[SUB]] * (SUB // 2), axis=0)


def recur(mixed, halo, keep, table, gate, taps_count):
    rows, chans = mixed.shape
    return pl.pallas_call(
        functools.partial(recur_kernel, taps_count),
        in_specs=[vmem()] * 5,
        out_specs=[vmem()] * 3,
        out_shape=[
            jax.ShapeDtypeStruct((rows, chans), F32),
            jax.ShapeDtypeStruct((rows, chans), F32),
            jax.ShapeDtypeStruct((3 * SUB, chans), F32),
        ],
        scratch_shapes=[
            pltpu.VMEM((rows + (taps_count - 1) * SUB, chans), F32),
            pltpu.VMEM((rows, chans), BF16),
            pltpu.VMEM((rows, 2 * chans), F32),
        ],
        compiler_params=params(),
        name="recur",
    )(mixed, halo, keep, table, gate)


def hidden_kernel(cum_ref, state_ref, head_ref, *refs):
    segment_refs, hidden_ref = refs[:-1], refs[-1]
    rows, chans = cum_ref.shape
    carried = jnp.zeros((1, chans), F32)
    for segment_ref in segment_refs:
        carried = carried * segment_ref[0:1, :] + segment_ref[1:2, :]
    entering = head_ref[SUB : 2 * SUB, :] + head_ref[0:SUB, :] * carried
    tile = 64
    wide = jnp.concatenate([entering] * (tile // SUB), axis=0)

    def step_of(step, _):
        at = pl.multiple_of(step * tile, tile)
        hidden_ref[pl.ds(at, tile), :] = (
            state_ref[pl.ds(at, tile), :] + cum_ref[pl.ds(at, tile), :] * wide
        ).astype(BF16)
        return 0

    lax.fori_loop(0, rows // tile, step_of, 0)


def hidden_of(cum, state, head, segments):
    return pl.pallas_call(
        hidden_kernel,
        in_specs=[vmem()] * (3 + len(segments)),
        out_specs=vmem(),
        out_shape=jax.ShapeDtypeStruct(cum.shape, BF16),
        compiler_params=params(),
        name="hidden",
    )(cum, state, head, *segments)


def out_kernel(groups, *refs):
    h_refs, w_ref, y_ref = refs[:groups], refs[groups], refs[groups + 1]
    for z in range(w_ref.shape[0]):
        total = jnp.dot(h_refs[0][...], w_ref[z, 0], preferred_element_type=F32)
        for k in range(1, groups):
            total = total + jnp.dot(h_refs[k][...], w_ref[z, k], preferred_element_type=F32)
        y_ref[z] = total.astype(BF16)


def out_projection(pieces, w):
    rows, chans = pieces[0].shape
    slices, groups, _, width = w.shape
    tile = min(rows, 256)
    return pl.pallas_call(
        functools.partial(out_kernel, groups),
        grid=(rows // tile,),
        in_specs=[pl.BlockSpec((tile, chans), lambda i: (i, 0))] * groups
        + [pl.BlockSpec(w.shape, lambda i: (0, 0, 0, 0))],
        out_specs=pl.BlockSpec((slices, tile, width), lambda i: (0, i, 0)),
        out_shape=jax.ShapeDtypeStruct((slices, rows, width), BF16),
        compiler_params=params(),
        name="out_projection",
    )(*pieces, w)


def swapped(value, axis, count, k):
    return lax.ppermute(value, axis, [(i, i ^ k) for i in range(count)])


def passed_along(value, axis, count, distance):
    return lax.ppermute(value, axis, [(i, i + distance) for i in range(count - distance)])


def per_device(
    tokens, documents, norm_gain, in_weight, conv_taps, conv_bias, recur_gate, input_gate,
    recur_bias, input_bias, decay_param, out_weight,
):
    outer, inner, pair = lax.axis_size("so"), lax.axis_size("si"), lax.axis_size("tp")
    place = lax.axis_index("si")
    own_rows, features = tokens.shape
    layers, width, chan_width = in_weight.shape
    taps_count = conv_taps.shape[1]
    block_dim = recur_gate.shape[2]
    rows = own_rows * inner
    steps = rows // SUB
    parts = own_rows // steps
    chans = chan_width // inner
    blocks = chans // block_dim
    others = [place ^ k for k in range(inner)]

    def in_piece(layer):
        split = in_weight[layer].reshape(width, inner, chans)
        return jnp.stack([lax.dynamic_index_in_dim(split, o, 1, False) for o in others])

    def out_piece(layer):
        split = out_weight[layer].reshape(inner, chans, width)
        return jnp.stack([lax.dynamic_index_in_dim(split, o, 0, False) for o in others])

    whole_in, whole_out = [], []
    for layer in range(layers):
        whole_in.append(lax.all_gather(in_piece(layer), "so", axis=0))
        whole_out.append(lax.all_gather(out_piece(layer), "so", axis=0))

    send = tokens.reshape(parts, steps, outer, inner, width).transpose(3, 2, 1, 0, 4)
    got = lax.all_to_all(send, "si", 0, 0, tiled=True)
    state_x = got.transpose(1, 2, 0, 3, 4).reshape(outer, rows, width)

    docs = documents.astype(F32)
    received = jnp.stack([docs] + [swapped(docs, "si", inner, k) for k in range(1, inner)])
    docs = jnp.concatenate([lax.dynamic_index_in_dim(received, place ^ j, 0, False) for j in range(inner)])
    before = passed_along(docs[rows - taps_count + 1 :] + 1.0, "so", outer, 1) - 1.0
    ext_docs = jnp.concatenate([before, docs])
    keeps = [
        (ext_docs[taps_count - 1 - lag : taps_count - 1 - lag + rows] == docs).astype(F32)
        for lag in range(1, taps_count)
    ]
    keep = jnp.stack(keeps, axis=-1).reshape(SUB, steps, taps_count - 1)
    keep = keep.transpose(1, 0, 2).reshape(rows, taps_count - 1)

    def own(values):
        return lax.dynamic_slice_in_dim(values, place * chans, chans, -1)

    def diagonal(gate):
        gate = lax.dynamic_slice_in_dim(gate, place * blocks, blocks, 1)
        eye = jnp.eye(blocks, dtype=BF16)
        full = gate[:, :, :, None, :] * eye[None, :, None, :, None]
        return full.reshape(layers, chans, chans)

    gates = jnp.concatenate([diagonal(recur_gate), diagonal(input_gate)], axis=-1)
    slope = -RG_C * jax.nn.softplus(-own(decay_param))
    rows_of = [own(conv_bias), own(recur_bias), own(input_bias), slope]
    table = jnp.concatenate([own(conv_taps)] + [r[:, None] for r in rows_of], axis=1)
    gain = lax.dynamic_index_in_dim(norm_gain.reshape(layers, outer, inner, width), place, 2, True)

    addends = []
    for layer in range(layers):
        state_x, stat, partials = in_projection(state_x, addends, gain[layer], whole_in[layer])
        pieces = [partials[0]] + [swapped(partials[k], "si", inner, k) for k in range(1, inner)]
        stats = [stat] + [swapped(stat, "si", inner, k) for k in range(1, inner)]
        mixed, tail = mix(pieces, stats, features)
        halo = passed_along(tail, "so", outer, 1)
        cum, state, head = recur(mixed, halo, keep, table[layer], gates[layer], taps_count)
        segment = head[2 * SUB :]
        if outer <= 4:
            segments = [passed_along(segment, "so", outer, d) for d in range(outer - 1, 0, -1)]
        else:
            gathered = lax.all_gather(segment, "so")
            earlier = (jnp.arange(outer) < lax.axis_index("so"))[:, None, None]
            first = jnp.arange(SUB)[:, None] % 2 == 0
            gathered = jnp.where(earlier, gathered, jnp.where(first, 1.0, 0.0))
            segments = [gathered[d] for d in range(outer)]
        hidden = hidden_of(cum, state, head, segments)
        pieces = [hidden] + [swapped(hidden, "si", inner, k) for k in range(1, inner)]
        partial = out_projection(pieces, whole_out[layer])
        if pair == 2:
            addends = [partial, swapped(partial, "tp", pair, 1)]
        else:
            addends = [lax.psum(partial, "tp")]

    summed = addends[0].astype(F32)
    for addend in addends[1:]:
        summed = summed + addend.astype(F32)
    state_x = (state_x.astype(F32) + summed).astype(BF16)
    send = state_x.reshape(outer, steps, inner, parts, width).transpose(2, 3, 1, 0, 4)
    got = lax.all_to_all(send, "si", 0, 0, tiled=True)
    return got.transpose(1, 2, 3, 0, 4).reshape(own_rows, features)


def solution(mesh):
    count = mesh.shape["sp"]
    inner = 4
    split = Mesh(
        mesh.devices.reshape(count // inner, inner, mesh.shape["tp"]), ("so", "si", "tp")
    )
    sp = ("so", "si")
    return jax.shard_map(
        per_device,
        mesh=split,
        in_specs=(
            P(sp, None),
            P(sp),
            P(),
            P(None, sp, "tp"),
            P(None, None, "tp"),
            P(None, "tp"),
            P(None, "tp", None, None),
            P(None, "tp", None, None),
            P(None, "tp"),
            P(None, "tp"),
            P(None, "tp"),
            P(None, "tp", sp),
        ),
        out_specs=P(sp, None),
        check_vma=False,
    )
```
